256 devices in a mesh: row: 32 (over z, y), col: 8 (over x, core).
Axes of the slice: x: 4, y: 4, z: 8, core: 2. Of those that a mesh axis runs over, the one named last changes fastest.
Arguments:
- tokens: bfloat16 [2, 65536, 1024], P(None, 'row'), may hold values from -6 to 6
- norm_gain: float32 [1024], replicated, may hold values from 0.1 to 1.9
- w_fourier_in: bfloat16 [1024, 512], P(None, 'col'), may hold values from -0.1875 to 0.1875
- w_gate: bfloat16 [1024, 1024], replicated, may hold values from -0.1875 to 0.1875
- w_spectrum: bfloat16 [512, 1024], replicated, may hold values from -0.25 to 0.25
- w_output: bfloat16 [1024, 1024], P(None, 'col'), may hold values from -0.375 to 0.375
Outputs:
- block_output: bfloat16 [2, 65536, 1024], P(None, 'row', 'col')
The draws below stay inside these ranges and needn't reach their ends.
All inputs are finite; a program needn't handle non-finite values.
Results may differ from the reference program's by a relative error of at most 0.015.
Values may be sent and summed in bfloat16 or wider, within the bound.
A program may use at most 320 MiB of HBM per device.

```python
import jax
import jax.numpy as jnp
from jax import lax

D = 1024
GROUPS = 8
GROUP_WIDTH = 64
FOURIER_WIDTH = 512
SEQS = 2
SEQ = 65536


def block_scale(stream_key, dims, cuts, low, largest):
    gain, own = 1.0, jax.random.fold_in(stream_key, 6)
    for axis_at, parts in cuts:
        steps = jnp.exp(jax.random.uniform(jax.random.fold_in(own, axis_at), (parts,), jnp.float32, low / len(cuts), largest / len(cuts)))
        gain = gain * jnp.repeat(steps, dims[axis_at] // parts).reshape([-1 if axis == axis_at else 1 for axis in range(len(dims))])
    return gain


def normal_values(own_key, dims, spread, bound, split=(), held_as=jnp.bfloat16):
    values = jax.random.normal(own_key, dims, jnp.float32) * spread
    if len(split) > 0:
        values = block_scale(own_key, dims, split, -0.22, 0.18) * values
    return jnp.clip(values, min=-bound, max=bound).astype(held_as)


def setup_inputs(seed: int = 0) -> dict:
    key_list = jax.random.split(jax.random.key(seed), 7)
    return {
        "tokens": normal_values(key_list[0], (SEQS, SEQ, D), 1.0, 6.0, ((1, 32),)),
        "norm_gain": jnp.clip(1.0 + 0.18 * jax.random.normal(key_list[1], (D,), jnp.float32), 0.1, 1.9),
        "w_fourier_in": normal_values(key_list[2], (D, FOURIER_WIDTH), D ** -0.5, 0.1875, ((1, 8),)),
        "w_gate": normal_values(key_list[3], (D, D), D ** -0.5, 0.1875),
        "w_spectrum": normal_values(key_list[4], (FOURIER_WIDTH, D), FOURIER_WIDTH ** -0.5, 0.25),
        "w_output": normal_values(key_list[5], (D, D), (D // 4) ** -0.5, 0.375, ((1, 8),)),
    }


norm_eps = 1e-6


def reference(tokens, norm_gain, w_fourier_in, w_gate, w_spectrum, w_output):
    widened = tokens.astype(jnp.float32)
    inverse = lax.rsqrt(jnp.mean(widened * widened, axis=-1, keepdims=True) + norm_eps)
    normed = (widened * inverse * norm_gain).astype(jnp.bfloat16).reshape(SEQS * SEQ, D)
    fourier_in = jnp.dot(normed, w_fourier_in, preferred_element_type=jnp.float32).astype(jnp.bfloat16)
    grouped = fourier_in.astype(jnp.float32).reshape(SEQS, SEQ, GROUPS, GROUP_WIDTH)
    spectrum = jnp.real(jnp.fft.fft2(grouped, axes=(1, 3), norm="ortho")).astype(jnp.bfloat16)
    spectrum = spectrum.reshape(SEQS * SEQ, FOURIER_WIDTH)
    mixed_pre = jnp.dot(spectrum, w_spectrum, preferred_element_type=jnp.float32).astype(jnp.bfloat16)
    gate_pre = jnp.dot(normed, w_gate, preferred_element_type=jnp.float32)
    mixed = (jax.nn.sigmoid(gate_pre) * mixed_pre.astype(jnp.float32)).astype(jnp.bfloat16)
    block_output = jnp.dot(mixed, w_output, preferred_element_type=jnp.float32).astype(jnp.bfloat16)
    return block_output.reshape(SEQS, SEQ, D)
```

```python
import functools

import jax
import jax.numpy as jnp
import numpy as np
from jax import lax
from jax.experimental import pallas as pl
from jax.experimental.pallas import tpu as pltpu
from jax.sharding import PartitionSpec as P

GROUP = 64
ROWS = 32
COLS = 8
SEQ = 65536
RADIX = 256
EPS = 1e-06
MESH = pl.DeviceIdType.MESH
BF16 = jnp.bfloat16
F32 = jnp.float32


def angles(left, right, period):
    return 2.0 * np.pi * (np.outer(left, right) % period) / period


def tables():
    n = np.arange(GROUP)
    channel = np.zeros((32, 2, GROUP))
    channel[:, 0] = np.cos(angles(np.arange(32), n, GROUP))
    channel[:, 1] = -np.sin(angles(np.arange(32), n, GROUP))
    channel[0, 1] = np.cos(angles(np.array([32]), n, GROUP))[0]
    spread = np.einsum("jan,pr->japrn", channel, np.eye(8)).reshape(512, 512)
    p = np.arange(RADIX)
    first_cos = np.cos(angles(p, p, RADIX))
    first_sin = -np.sin(angles(p, p, RADIX))
    first = np.zeros((2, 2, RADIX, 32, 2, 8))
    for part in range(2):
        first[part, 0, :, :, part] = first_cos.reshape(RADIX, 32, 8)
        first[part, 1, :, :, part] = first_sin.reshape(RADIX, 32, 8)
    first = first.reshape(1024, 512)
    twist = angles(p, p, SEQ)
    twist = np.stack([np.cos(twist), np.sin(twist)])
    second_cos = np.cos(angles(p, p, RADIX)) / 2048.0
    second_sin = np.sin(angles(p, p, RADIX)) / 2048.0
    second = np.stack(
        [
            np.concatenate([second_cos, second_sin], axis=1),
            np.concatenate([second_sin, -second_cos], axis=1),
        ]
    )
    bf = lambda a: jnp.asarray(a, dtype=F32).astype(BF16)
    return bf(spread), bf(first), jnp.asarray(twist, dtype=F32), bf(second)


def dot(a, b):
    return jnp.dot(a, b, preferred_element_type=F32)


def dot_nt(a, b):
    return lax.dot_general(a, b, (((1,), (1,)), ((), ())), preferred_element_type=F32)


def kernel(
    tok, gain, wfin, wgate, wspec, wout, spread, first, twist, second,
    out,
    x_v, gain_v, wfin_v, wgate_v, wspec_v, wout_v, spread_v, first_v, twist_v, second_v,
    wg_v, u_v, sig_v, perm_v, eye_v,
    send1, recv1, send2, recv2, send3, recv3, send4,
    x_sem, w_sem, ssem, rsem, wo_s, wo_r,
):
    row = lax.axis_index("row")
    col = lax.axis_index("col")
    chip = col // 2
    core = col % 2
    mate = chip * 2 + (1 - core)
    bar = pltpu.get_barrier_semaphore()

    def row_peer(d):
        return lax.rem(row + d, ROWS)

    def col_peer(d):
        return lax.rem(col + d, COLS)

    def signal_row(d, c):
        pl.semaphore_signal(bar, inc=1, device_id=(row_peer(d), col), device_id_type=MESH)
        return c

    def signal_col(d, c):
        pl.semaphore_signal(bar, inc=1, device_id=(row, col_peer(d)), device_id_type=MESH)
        return c

    lax.fori_loop(1, ROWS, signal_row, 0)
    lax.fori_loop(1, COLS, signal_col, 0)

    my_cols = pl.ds(pl.multiple_of(col * 128, 128), 128)
    loads = [
        pltpu.make_async_copy(gain, gain_v, w_sem.at[0]),
        pltpu.make_async_copy(wfin, wfin_v, w_sem.at[1]),
        pltpu.make_async_copy(spread, spread_v, w_sem.at[2]),
        pltpu.make_async_copy(wout, wout_v.at[:, my_cols], w_sem.at[3]),
        pltpu.make_async_copy(first, first_v, w_sem.at[4]),
        pltpu.make_async_copy(twist, twist_v, w_sem.at[5]),
        pltpu.make_async_copy(second, second_v, w_sem.at[6]),
        pltpu.make_async_copy(wgate, wgate_v, w_sem.at[7]),
        pltpu.make_async_copy(wspec, wspec_v, w_sem.at[8]),
    ]

    def tok_copy(b, i):
        return pltpu.make_async_copy(
            tok.at[b, pl.ds(pl.multiple_of(i * 512, 512), 512), :], x_v.at[b, i], x_sem.at[b, i]
        )

    loads[0].start()
    loads[1].start()
    for i in range(4):
        tok_copy(0, i).start()
    for i in (2, 3, 4, 5, 6):
        loads[i].start()
    for i in range(4):
        tok_copy(1, i).start()
    loads[7].start()
    loads[8].start()

    loads[0].wait()
    loads[1].wait()
    gain_col = jnp.transpose(jnp.broadcast_to(gain_v[...], (8, 1024)))[:, 0:1]
    wg_v[...] = (wfin_v[...].astype(F32) * gain_col).astype(BF16)

    def project(b):
        def body(i, c):
            tok_copy(b, i).wait()
            halves = []
            for h in range(2):
                x = x_v[b, i, pl.ds(h * 256, 256), :]
                wide = x.astype(F32)
                inv = lax.rsqrt(jnp.sum(wide * wide, axis=1, keepdims=True) * (1.0 / 1024) + EPS)
                halves.append(dot(x, wg_v[...]) * inv)
            u_v[b, :, pl.ds(pl.multiple_of(i * 128, 128), 128)] = jnp.concatenate(
                halves, axis=1
            ).astype(BF16)
            return c

        lax.fori_loop(0, 4, body, 0)
        send1[b] = dot_nt(spread_v[...], u_v[b]).astype(BF16)

    def rows16(i):
        return pl.ds(pl.multiple_of(i * 16, 16), 16)

    def row_exchange(src, dst, b, k):
        def send(d, c):
            t = row_peer(d)
            pltpu.make_async_remote_copy(
                src_ref=src.at[b, rows16(t), :],
                dst_ref=dst.at[b, rows16(row), :],
                send_sem=ssem.at[k, b],
                recv_sem=rsem.at[k, b],
                device_id=(t, col),
                device_id_type=MESH,
            ).start()
            return c

        lax.fori_loop(1, ROWS, send, 0)
        dst[b, rows16(row), :] = src[b, rows16(row), :]

    def row_wait(ref, sem, b):
        part = ref.at[b, pl.ds(0, 16 * (ROWS - 1)), :]
        pltpu.make_async_copy(part, part, sem).wait()

    loads[2].wait()
    project(0)
    pl.semaphore_wait(bar, ROWS - 1 + COLS - 1)
    row_exchange(send1, recv1, 0, 0)

    def wout_copy(source, target, sem):
        block = wout_v.at[:, pl.ds(pl.multiple_of(source * 128, 128), 128)]
        return pltpu.make_async_remote_copy(
            src_ref=block,
            dst_ref=block,
            send_sem=wo_s.at[sem],
            recv_sem=wo_r.at[sem],
            device_id=(row, target),
            device_id_type=MESH,
        )

    loads[3].wait()
    for d in (1, 3, 2):
        wout_copy(col, lax.rem(chip + d, 4) * 2 + core, 0).start()
    wout_copy(col, mate, 1).start()

    project(1)
    row_exchange(send1, recv1, 1, 0)

    perm_row = lax.broadcasted_iota(jnp.int32, (512, 512), 0)
    perm_col = lax.broadcasted_iota(jnp.int32, (512, 512), 1)
    pair = perm_col // 16
    chan = jnp.where(perm_col % 16 < 8, pair, jnp.where(pair == 0, 32, 64 - pair))
    perm_v[...] = jnp.where(perm_row == (perm_col % 8) * 64 + chan, 1.0, 0.0).astype(BF16)
    eye_v[...] = jnp.where(
        lax.broadcasted_iota(jnp.int32, (256, 256), 0)
        == lax.broadcasted_iota(jnp.int32, (256, 256), 1),
        1.0,
        0.0,
    ).astype(BF16)

    loads[7].wait()
    for b in range(2):
        wide = x_v[b, col // 2, pl.ds(pl.multiple_of((col % 2) * 256, 256), 256), :].astype(F32)
        inv = lax.rsqrt(jnp.sum(wide * wide, axis=1, keepdims=True) * (1.0 / 1024) + EPS)
        normed = (wide * inv * gain_v[...]).astype(BF16)
        sig_v[b] = jax.nn.sigmoid(dot(normed, wgate_v[...]))

    loads[4].wait()
    loads[5].wait()
    loads[6].wait()
    plain = row != 0
    mix01 = jnp.where(plain, 1.0, 0.0).astype(F32)
    mix11 = jnp.where(plain, -1.0, 1.0).astype(F32)
    odd = jnp.where(plain, 1, 0)

    def transform(b):
        section = dot(first_v[...], recv1[b])
        c = twist_v[0]
        s = twist_v[1]

        def turned(re, im):
            return jnp.concatenate([re * c + im * s, im * c - re * s], axis=1).astype(BF16)

        even_part = dot_nt(second_v[0], turned(section[0:256], section[256:512]))
        odd_part = dot_nt(second_v[odd], turned(section[512:768], section[768:1024]))
        one = even_part + mix01 * odd_part
        two = mix01 * even_part + mix11 * odd_part
        send2[b] = (
            jnp.concatenate([one.reshape(32, 8, 256), two.reshape(32, 8, 256)], axis=1)
            .reshape(512, 256)
            .astype(BF16)
        )

    for b in range(2):
        row_wait(recv1, rsem.at[0, b], b)
        transform(b)
        row_exchange(send2, recv2, b, 1)

    got = wout_v.at[:, pl.ds(0, 384)]
    pltpu.make_async_copy(got, got, wo_r.at[0]).wait()
    for d in (1, 2, 3):
        wout_copy(lax.rem(chip + d, 4) * 2 + core, mate, 1).start()

    def rows64(i):
        return pl.ds(pl.multiple_of(i * 64, 64), 64)

    def spread_tokens(b):
        row_wait(recv2, rsem.at[1, b], b)
        send3[b] = dot(perm_v[...], recv2[b]).astype(BF16)

        def send(d, c):
            t = col_peer(d)
            pltpu.make_async_remote_copy(
                src_ref=send3.at[b, rows64(t), :],
                dst_ref=recv3.at[b, rows64(col), :],
                send_sem=ssem.at[2, b],
                recv_sem=rsem.at[2, b],
                device_id=(row, t),
                device_id_type=MESH,
            ).start()
            return c

        lax.fori_loop(1, COLS, send, 0)
        recv3[b, rows64(col), :] = send3[b, rows64(col), :]

    def finish(b):
        part = recv3.at[b, pl.ds(0, 448), :]
        pltpu.make_async_copy(part, part, rsem.at[2, b]).wait()
        spectrum = dot_nt(eye_v[...], recv3[b]).astype(BF16)
        mixed_pre = dot(spectrum, wspec_v[...]).astype(BF16).astype(F32)
        mixed = (sig_v[b] * mixed_pre).astype(BF16)
        result = dot(mixed, wout_v[...]).astype(BF16)
        for t in range(COLS):
            send4[b, t] = result[:, t * 128 : (t + 1) * 128]

        def send(d, c):
            t = col_peer(d)
            pltpu.make_async_remote_copy(
                src_ref=send4.at[b, t],
                dst_ref=out.at[b, pl.ds(pl.multiple_of(col * 256, 256), 256), :],
                send_sem=ssem.at[3, b],
                recv_sem=rsem.at[3, b],
                device_id=(row, t),
                device_id_type=MESH,
            ).start()
            return c

        lax.fori_loop(1, COLS, send, 0)
        out[b, pl.ds(pl.multiple_of(col * 256, 256), 256), :] = send4[b, col]

    spread_tokens(0)
    loads[8].wait()
    mates = wout_v.at[:, pl.ds(0, 512)]
    pltpu.make_async_copy(mates, mates, wo_r.at[1]).wait()
    finish(0)
    spread_tokens(1)
    finish(1)

    for b in range(2):
        part = out.at[b, pl.ds(0, 1792), :]
        pltpu.make_async_copy(part, part, rsem.at[3, b]).wait()
        row_wait(send1, ssem.at[0, b], b)
        row_wait(send2, ssem.at[1, b], b)
        part = send3.at[b, pl.ds(0, 448), :]
        pltpu.make_async_copy(part, part, ssem.at[2, b]).wait()
        part = send4.at[b, pl.ds(0, 7)]
        pltpu.make_async_copy(part, part, ssem.at[3, b]).wait()
    pltpu.make_async_copy(got, got, wo_s.at[0]).wait()
    pltpu.make_async_copy(mates, mates, wo_s.at[1]).wait()


def on_device(tokens, norm_gain, w_fourier_in, w_gate, w_spectrum, w_output):
    spread, first, twist, second = tables()
    vmem = pltpu.VMEM
    return pl.pallas_call(
        kernel,
        out_shape=jax.ShapeDtypeStruct((2, 2048, 128), BF16),
        in_specs=[pl.BlockSpec(memory_space=pl.ANY)] * 10,
        out_specs=pl.BlockSpec(memory_space=pltpu.VMEM),
        scratch_shapes=[
            vmem((2, 4, 512, 1024), BF16),
            vmem((1, 1024), F32),
            vmem((1024, 64), BF16),
            vmem((1024, 1024), BF16),
            vmem((512, 1024), BF16),
            vmem((1024, 1024), BF16),
            vmem((512, 512), BF16),
            vmem((1024, 512), BF16),
            vmem((2, 256, 256), F32),
            vmem((2, 256, 512), BF16),
            vmem((1024, 64), BF16),
            vmem((2, 256, 512), BF16),
            vmem((2, 256, 1024), F32),
            vmem((512, 512), BF16),
            vmem((256, 256), BF16),
            vmem((2, 512, 256), BF16),
            vmem((2, 512, 256), BF16),
            vmem((2, 512, 256), BF16),
            vmem((2, 512, 256), BF16),
            vmem((2, 512, 256), BF16),
            vmem((2, 512, 256), BF16),
            vmem((2, 8, 256, 128), BF16),
            pltpu.SemaphoreType.DMA((2, 4)),
            pltpu.SemaphoreType.DMA((9,)),
            pltpu.SemaphoreType.DMA((4, 2)),
            pltpu.SemaphoreType.DMA((4, 2)),
            pltpu.SemaphoreType.DMA((2,)),
            pltpu.SemaphoreType.DMA((2,)),
        ],
        compiler_params=pltpu.CompilerParams(
            collective_id=0, has_side_effects=True, vmem_limit_bytes=60 << 20
        ),
    )(
        tokens, norm_gain.reshape(1, 1024), w_fourier_in, w_gate, w_spectrum, w_output,
        spread, first, twist, second,
    )


def solution(mesh):
    placed = (P(None, "row", None), P(), P(None, "col"), P(), P(), P(None, "col"))
    return jax.shard_map(
        on_device, mesh=mesh, in_specs=placed, out_specs=P(None, "row", "col"), check_vma=False
    )
```

```python
import functools

import jax
import jax.numpy as jnp
import numpy as np
from jax import lax
from jax.experimental import pallas as pl
from jax.experimental.pallas import tpu as pltpu
from jax.sharding import PartitionSpec as P

GROUP = 64
ROWS = 32
COLS = 8
SEQ = 65536
RADIX = 256
EPS = 1e-06
MESH = pl.DeviceIdType.MESH
BF16 = jnp.bfloat16
F32 = jnp.float32


def angles(left, right, period):
    return 2.0 * np.pi * (np.outer(left, right) % period) / period


def tables():
    n = np.arange(GROUP)
    channel = np.zeros((32, 2, GROUP))
    channel[:, 0] = np.cos(angles(np.arange(32), n, GROUP))
    channel[:, 1] = -np.sin(angles(np.arange(32), n, GROUP))
    channel[0, 1] = np.cos(angles(np.array([32]), n, GROUP))[0]
    spread = np.einsum("jan,pr->japrn", channel, np.eye(8)).reshape(512, 512)
    p = np.arange(RADIX)
    first_cos = np.cos(angles(p, p, RADIX))
    first_sin = -np.sin(angles(p, p, RADIX))
    first = np.zeros((2, 2, RADIX, 32, 2, 8))
    for part in range(2):
        first[part, 0, :, :, part] = first_cos.reshape(RADIX, 32, 8)
        first[part, 1, :, :, part] = first_sin.reshape(RADIX, 32, 8)
    first = first.reshape(1024, 512)
    twist = angles(p, p, SEQ)
    twist = np.stack([np.cos(twist), np.sin(twist)])
    second_cos = np.cos(angles(p, p, RADIX)) / 2048.0
    second_sin = np.sin(angles(p, p, RADIX)) / 2048.0
    second = np.stack(
        [
            np.concatenate([second_cos, second_sin], axis=1),
            np.concatenate([second_sin, -second_cos], axis=1),
        ]
    )
    bf = lambda a: jnp.asarray(a, dtype=F32).astype(BF16)
    return bf(spread), bf(first), jnp.asarray(twist, dtype=F32), bf(second)


def dot(a, b):
    return jnp.dot(a, b, preferred_element_type=F32)


def dot_nt(a, b):
    return lax.dot_general(a, b, (((1,), (1,)), ((), ())), preferred_element_type=F32)


def kernel(
    tok, gain, wfin, wgate, wspec, wout, spread, first, twist, second,
    out,
    x_v, gain_v, wfin_v, wgate_v, wspec_v, wout_v, spread_v, first_v, twist_v, second_v,
    wg_v, u_v, sig_v, perm_v, eye_v,
    send1, recv1, send2, recv2, send3, recv3, send4,
    x_sem, w_sem, s1, r1, s2, r2, s3, r3, s4, r4, wo_s, wo_r,
):
    row = lax.axis_index("row")
    col = lax.axis_index("col")
    chip = col // 2
    core = col % 2
    mate = chip * 2 + (1 - core)
    bar = pltpu.get_barrier_semaphore()

    def row_peer(d):
        return lax.rem(row + d, ROWS)

    def col_peer(d):
        return lax.rem(col + d, COLS)

    def signal_row(d, c):
        pl.semaphore_signal(bar, inc=1, device_id=(row_peer(d), col), device_id_type=MESH)
        return c

    def signal_col(d, c):
        pl.semaphore_signal(bar, inc=1, device_id=(row, col_peer(d)), device_id_type=MESH)
        return c

    lax.fori_loop(1, ROWS, signal_row, 0)
    lax.fori_loop(1, COLS, signal_col, 0)

    my_cols = pl.ds(pl.multiple_of(col * 128, 128), 128)
    loads = [
        pltpu.make_async_copy(gain, gain_v, w_sem.at[0]),
        pltpu.make_async_copy(wfin, wfin_v, w_sem.at[1]),
        pltpu.make_async_copy(spread, spread_v, w_sem.at[2]),
        pltpu.make_async_copy(wout, wout_v.at[:, my_cols], w_sem.at[3]),
        pltpu.make_async_copy(first, first_v, w_sem.at[4]),
        pltpu.make_async_copy(twist, twist_v, w_sem.at[5]),
        pltpu.make_async_copy(second, second_v, w_sem.at[6]),
        pltpu.make_async_copy(wgate, wgate_v, w_sem.at[7]),
        pltpu.make_async_copy(wspec, wspec_v, w_sem.at[8]),
    ]

    def tok_copy(b, i):
        return pltpu.make_async_copy(
            tok.at[b, pl.ds(pl.multiple_of(i * 512, 512), 512), :], x_v.at[b, i], x_sem.at[b, i]
        )

    loads[0].start()
    loads[1].start()
    for i in range(4):
        tok_copy(0, i).start()
    for i in (2, 3, 4, 5, 6):
        loads[i].start()
    for i in range(4):
        tok_copy(1, i).start()
    loads[7].start()
    loads[8].start()

    loads[0].wait()
    loads[1].wait()
    wg_v[...] = (wfin_v[...].astype(F32) * gain_v[...]).astype(BF16)

    def project(b):
        def body(i, c):
            tok_copy(b, i).wait()
            halves = []
            for h in range(2):
                x = x_v[b, i, pl.ds(h * 256, 256), :]
                wide = x.astype(F32)
                inv = lax.rsqrt(jnp.sum(wide * wide, axis=1, keepdims=True) * (1.0 / 1024) + EPS)
                halves.append(dot_nt(x, wg_v[...]) * inv)
            u_v[b, :, pl.ds(pl.multiple_of(i * 128, 128), 128)] = jnp.concatenate(
                halves, axis=1
            ).astype(BF16)
            return c

        lax.fori_loop(0, 4, body, 0)
        send1[b] = dot_nt(spread_v[...], u_v[b]).astype(BF16)

    def rows16(i):
        return pl.ds(pl.multiple_of(i * 16, 16), 16)

    def row_exchange(src, dst, send_sem, recv_sem):
        def send(d, c):
            t = row_peer(d)
            pltpu.make_async_remote_copy(
                src_ref=src.at[rows16(t), :],
                dst_ref=dst.at[rows16(row), :],
                send_sem=send_sem,
                recv_sem=recv_sem,
                device_id=(t, col),
                device_id_type=MESH,
            ).start()
            return c

        lax.fori_loop(1, ROWS, send, 0)
        dst[rows16(row), :] = src[rows16(row), :]

    def wait_for(part, sem):
        pltpu.make_async_copy(part, part, sem).wait()

    def row_wait(ref, sem):
        wait_for(ref.at[pl.ds(0, 16 * (ROWS - 1)), :], sem)

    loads[2].wait()
    project(0)
    pl.semaphore_wait(bar, ROWS - 1 + COLS - 1)
    row_exchange(send1.at[0], recv1.at[0], s1.at[0], r1.at[0])

    def wout_copy(source, target, sem):
        block = wout_v.at[:, pl.ds(pl.multiple_of(source * 128, 128), 128)]
        return pltpu.make_async_remote_copy(
            src_ref=block,
            dst_ref=block,
            send_sem=wo_s.at[sem],
            recv_sem=wo_r.at[sem],
            device_id=(row, target),
            device_id_type=MESH,
        )

    loads[3].wait()
    for d in (1, 3, 2):
        wout_copy(col, lax.rem(chip + d, 4) * 2 + core, 0).start()
    wout_copy(col, mate, 1).start()

    project(1)
    row_exchange(send1.at[1], recv1.at[1], s1.at[1], r1.at[1])

    perm_row = lax.broadcasted_iota(jnp.int32, (512, 512), 0)
    perm_col = lax.broadcasted_iota(jnp.int32, (512, 512), 1)
    pair = perm_col // 16
    chan = jnp.where(perm_col % 16 < 8, pair, jnp.where(pair == 0, 32, 64 - pair))
    perm_v[...] = jnp.where(perm_row == (perm_col % 8) * 64 + chan, 1.0, 0.0).astype(BF16)
    eye_v[...] = jnp.where(
        lax.broadcasted_iota(jnp.int32, (128, 128), 0)
        == lax.broadcasted_iota(jnp.int32, (128, 128), 1),
        1.0,
        0.0,
    ).astype(BF16)

    loads[7].wait()
    for b in range(2):
        wide = x_v[b, col // 2, pl.ds(pl.multiple_of((col % 2) * 256, 256), 256), :].astype(F32)
        inv = lax.rsqrt(jnp.sum(wide * wide, axis=1, keepdims=True) * (1.0 / 1024) + EPS)
        normed = (wide * inv * gain_v[...]).astype(BF16)
        sig_v[b] = jax.nn.sigmoid(dot(normed, wgate_v[...]))

    loads[4].wait()
    loads[5].wait()
    loads[6].wait()
    plain = row != 0
    mix01 = jnp.where(plain, 1.0, 0.0).astype(F32)
    mix11 = jnp.where(plain, -1.0, 1.0).astype(F32)
    odd = jnp.where(plain, 1, 0)

    def transform(b):
        section = dot(first_v[...], recv1[b])
        c = twist_v[0]
        s = twist_v[1]

        def turned(re, im):
            return jnp.concatenate([re * c + im * s, im * c - re * s], axis=1).astype(BF16)

        even_part = dot_nt(second_v[0], turned(section[0:256], section[256:512]))
        odd_part = dot_nt(second_v[odd], turned(section[512:768], section[768:1024]))
        one = even_part + mix01 * odd_part
        two = mix01 * even_part + mix11 * odd_part
        both = (
            jnp.concatenate([one.reshape(32, 8, 256), two.reshape(32, 8, 256)], axis=1)
            .reshape(512, 256)
            .astype(BF16)
        )
        for h in range(2):
            send2[b, h] = both[:, h * 128 : (h + 1) * 128]

    for b in range(2):
        row_wait(recv1.at[b], r1.at[b])
        transform(b)
        for h in range(2):
            row_exchange(send2.at[b, h], recv2.at[b, h], s2.at[b, h], r2.at[b, h])

    wait_for(wout_v.at[:, pl.ds(0, 384)], wo_r.at[0])
    for d in (1, 2, 3):
        wout_copy(lax.rem(chip + d, 4) * 2 + core, mate, 1).start()

    def rows64(i):
        return pl.ds(pl.multiple_of(i * 64, 64), 64)

    def spread_tokens(b, h):
        row_wait(recv2.at[b, h], r2.at[b, h])
        send3[b, h] = dot(perm_v[...], recv2[b, h]).astype(BF16)

        def send(d, c):
            t = col_peer(d)
            pltpu.make_async_remote_copy(
                src_ref=send3.at[b, h, rows64(t), :],
                dst_ref=recv3.at[b, h, rows64(col), :],
                send_sem=s3.at[b, h],
                recv_sem=r3.at[b, h],
                device_id=(row, t),
                device_id_type=MESH,
            ).start()
            return c

        lax.fori_loop(1, COLS, send, 0)
        recv3[b, h, rows64(col), :] = send3[b, h, rows64(col), :]

    def finish(b, h):
        wait_for(recv3.at[b, h, pl.ds(0, 448), :], r3.at[b, h])
        spectrum = dot_nt(eye_v[...], recv3[b, h]).astype(BF16)
        mixed_pre = dot(spectrum, wspec_v[...]).astype(BF16).astype(F32)
        mixed = (sig_v[b, h * 128 : (h + 1) * 128] * mixed_pre).astype(BF16)
        result = dot(mixed, wout_v[...]).astype(BF16)
        for t in range(COLS):
            send4[b, h, t] = result[:, t * 128 : (t + 1) * 128]
        place = pl.ds(pl.multiple_of(col * 256 + h * 128, 128), 128)

        def send(d, c):
            t = col_peer(d)
            pltpu.make_async_remote_copy(
                src_ref=send4.at[b, h, t],
                dst_ref=out.at[b, place, :],
                send_sem=s4.at[b, h],
                recv_sem=r4.at[b, h],
                device_id=(row, t),
                device_id_type=MESH,
            ).start()
            return c

        lax.fori_loop(1, COLS, send, 0)
        out[b, place, :] = send4[b, h, col]

    spread_tokens(0, 0)
    loads[8].wait()
    wait_for(wout_v.at[:, pl.ds(0, 512)], wo_r.at[1])
    spread_tokens(0, 1)
    finish(0, 0)
    spread_tokens(1, 0)
    finish(0, 1)
    spread_tokens(1, 1)
    finish(1, 0)
    finish(1, 1)

    for b in range(2):
        row_wait(send1.at[b], s1.at[b])
        for h in range(2):
            row_wait(send2.at[b, h], s2.at[b, h])
            wait_for(send3.at[b, h, pl.ds(0, 448), :], s3.at[b, h])
            wait_for(send4.at[b, h, pl.ds(0, 7)], s4.at[b, h])
            wait_for(out.at[b, pl.ds(0, 896), :], r4.at[b, h])
    wait_for(wout_v.at[:, pl.ds(0, 384)], wo_s.at[0])
    wait_for(wout_v.at[:, pl.ds(0, 512)], wo_s.at[1])


def on_device(tokens, norm_gain, w_fourier_in, w_gate, w_spectrum, w_output):
    spread, first, twist, second = tables()
    vmem = pltpu.VMEM
    return pl.pallas_call(
        kernel,
        out_shape=vmem((2, 2048, 128), BF16),
        in_specs=[pl.BlockSpec(memory_space=pl.ANY)] * 10,
        out_specs=pl.BlockSpec(memory_space=pltpu.VMEM),
        scratch_shapes=[
            vmem((2, 4, 512, 1024), BF16),
            vmem((1, 1024), F32),
            vmem((64, 1024), BF16),
            vmem((1024, 1024), BF16),
            vmem((512, 1024), BF16),
            vmem((1024, 1024), BF16),
            vmem((512, 512), BF16),
            vmem((1024, 512), BF16),
            vmem((2, 256, 256), F32),
            vmem((2, 256, 512), BF16),
            vmem((64, 1024), BF16),
            vmem((2, 256, 512), BF16),
            vmem((2, 256, 1024), F32),
            vmem((512, 512), BF16),
            vmem((128, 128), BF16),
            vmem((2, 512, 256), BF16),
            vmem((2, 512, 256), BF16),
            *[vmem((2, 2, 512, 128), BF16)] * 4,
            vmem((2, 2, 8, 128, 128), BF16),
            pltpu.SemaphoreType.DMA((2, 4)),
            pltpu.SemaphoreType.DMA((9,)),
            pltpu.SemaphoreType.DMA((2,)),
            pltpu.SemaphoreType.DMA((2,)),
            *[pltpu.SemaphoreType.DMA((2, 2))] * 6,
            pltpu.SemaphoreType.DMA((2,)),
            pltpu.SemaphoreType.DMA((2,)),
        ],
        compiler_params=pltpu.CompilerParams(
            collective_id=0, has_side_effects=True, vmem_limit_bytes=60 << 20
        ),
    )(
        tokens, norm_gain.reshape(1, 1024), w_fourier_in.T, w_gate, w_spectrum, w_output,
        spread, first, twist, second,
    )


def solution(mesh):
    placed = (P(None, "row", None), P(), P(None, "col"), P(), P(), P(None, "col"))
    return jax.shard_map(
        on_device, mesh=mesh, in_specs=placed, out_specs=P(None, "row", "col"), check_vma=False
    )
```

```python
import functools

import jax
import jax.numpy as jnp
import numpy as np
from jax import lax
from jax.experimental import pallas as pl
from jax.experimental.pallas import tpu as pltpu
from jax.sharding import PartitionSpec as P

GROUP = 64
ROWS = 32
COLS = 8
SEQ = 65536
RADIX = 256
EPS = 1e-06
MESH = pl.DeviceIdType.MESH
BF16 = jnp.bfloat16
F32 = jnp.float32


def angles(left, right, period):
    return 2.0 * np.pi * (np.outer(left, right) % period) / period


def tables():
    n = np.arange(GROUP)
    channel = np.zeros((32, 2, GROUP))
    channel[:, 0] = np.cos(angles(np.arange(32), n, GROUP))
    channel[:, 1] = -np.sin(angles(np.arange(32), n, GROUP))
    channel[0, 1] = np.cos(angles(np.array([32]), n, GROUP))[0]
    spread = np.einsum("jan,pr->japrn", channel, np.eye(8)).reshape(512, 512)
    p = np.arange(RADIX)
    first_cos = np.cos(angles(p, p, RADIX))
    first_sin = -np.sin(angles(p, p, RADIX))
    first = np.zeros((2, 2, RADIX, 32, 2, 8))
    for part in range(2):
        first[part, 0, :, :, part] = first_cos.reshape(RADIX, 32, 8)
        first[part, 1, :, :, part] = first_sin.reshape(RADIX, 32, 8)
    first = first.reshape(1024, 512)
    twist = angles(p, p, SEQ)
    twist = np.stack([np.cos(twist), np.sin(twist)])
    second_cos = np.cos(angles(p, p, RADIX)) / 2048.0
    second_sin = np.sin(angles(p, p, RADIX)) / 2048.0
    second = np.stack(
        [
            np.concatenate([second_cos, second_sin], axis=1),
            np.concatenate([second_sin, -second_cos], axis=1),
        ]
    )
    second = second.reshape(2, 32, 8, 512).transpose(0, 2, 1, 3).reshape(2, 256, 512)
    bf = lambda a: jnp.asarray(a, dtype=F32).astype(BF16)
    return bf(spread), bf(first), jnp.asarray(twist, dtype=F32), bf(second)


def dot(a, b):
    return jnp.dot(a, b, preferred_element_type=F32)


def dot_nt(a, b):
    return lax.dot_general(a, b, (((1,), (1,)), ((), ())), preferred_element_type=F32)


def kernel(
    tok, gain, wfin, wgate, wspec, wout, spread, first, twist, second,
    out,
    x_v, gain_v, wfin_v, wgate_v, wspec_v, wspec_p, wout_v, spread_v, first_v, twist_v, second_v,
    wg_v, u_v, sig_v, perm_v, eye_v,
    send1, recv1, send2, recv2, send3, recv3, send4,
    x_sem, w_sem, s1, r1, s2, r2, s3, r3, s4, r4, wo_s, wo_r,
):
    row = lax.axis_index("row")
    col = lax.axis_index("col")
    chip = col // 2
    core = col % 2
    mate = chip * 2 + (1 - core)
    bar = pltpu.get_barrier_semaphore()

    def row_peer(d):
        return lax.rem(row + d, ROWS)

    def col_peer(d):
        return lax.rem(col + d, COLS)

    def signal_row(d, c):
        pl.semaphore_signal(bar, inc=1, device_id=(row_peer(d), col), device_id_type=MESH)
        return c

    def signal_col(d, c):
        pl.semaphore_signal(bar, inc=1, device_id=(row, col_peer(d)), device_id_type=MESH)
        return c

    lax.fori_loop(1, ROWS, signal_row, 0)
    lax.fori_loop(1, COLS, signal_col, 0)

    my_cols = pl.ds(pl.multiple_of(col * 128, 128), 128)
    loads = [
        pltpu.make_async_copy(gain, gain_v, w_sem.at[0]),
        pltpu.make_async_copy(wfin, wfin_v, w_sem.at[1]),
        pltpu.make_async_copy(spread, spread_v, w_sem.at[2]),
        pltpu.make_async_copy(wout, wout_v.at[:, my_cols], w_sem.at[3]),
        pltpu.make_async_copy(first, first_v, w_sem.at[4]),
        pltpu.make_async_copy(twist, twist_v, w_sem.at[5]),
        pltpu.make_async_copy(second, second_v, w_sem.at[6]),
        pltpu.make_async_copy(wgate, wgate_v, w_sem.at[7]),
        pltpu.make_async_copy(wspec, wspec_v, w_sem.at[8]),
    ]

    def tok_copy(b, i):
        return pltpu.make_async_copy(
            tok.at[b, pl.ds(pl.multiple_of(i * 512, 512), 512), :], x_v.at[b, i], x_sem.at[b, i]
        )

    loads[0].start()
    loads[1].start()
    for i in range(4):
        tok_copy(0, i).start()
    for i in (2, 3, 4, 5, 6):
        loads[i].start()
    for i in range(4):
        tok_copy(1, i).start()
    loads[7].start()
    loads[8].start()

    loads[0].wait()
    loads[1].wait()
    wg_v[...] = (wfin_v[...].astype(F32) * gain_v[...]).astype(BF16)

    def project(b):
        def body(i, c):
            tok_copy(b, i).wait()
            halves = []
            for h in range(2):
                x = x_v[b, i, pl.ds(h * 256, 256), :]
                wide = x.astype(F32)
                inv = lax.rsqrt(jnp.sum(wide * wide, axis=1, keepdims=True) * (1.0 / 1024) + EPS)
                halves.append(dot_nt(x, wg_v[...]) * inv)
            u_v[b, :, pl.ds(pl.multiple_of(i * 128, 128), 128)] = jnp.concatenate(
                halves, axis=1
            ).astype(BF16)
            return c

        lax.fori_loop(0, 4, body, 0)
        send1[b] = dot_nt(spread_v[...], u_v[b]).astype(BF16)

    def rows16(i):
        return pl.ds(pl.multiple_of(i * 16, 16), 16)

    def row_exchange(src, dst, send_sem, recv_sem):
        def send(d, c):
            t = row_peer(d)
            pltpu.make_async_remote_copy(
                src_ref=src.at[rows16(t), :],
                dst_ref=dst.at[rows16(row), :],
                send_sem=send_sem,
                recv_sem=recv_sem,
                device_id=(t, col),
                device_id_type=MESH,
            ).start()
            return c

        lax.fori_loop(1, ROWS, send, 0)
        dst[rows16(row), :] = src[rows16(row), :]

    def wait_for(part, sem):
        pltpu.make_async_copy(part, part, sem).wait()

    def row_wait(ref, sem):
        wait_for(ref.at[pl.ds(0, 16 * (ROWS - 1)), :], sem)

    loads[2].wait()
    project(0)
    pl.semaphore_wait(bar, ROWS - 1 + COLS - 1)
    row_exchange(send1.at[0], recv1.at[0], s1.at[0], r1.at[0])

    def wout_copy(part, source, target, sem):
        block = wout_v.at[part, pl.ds(pl.multiple_of(source * 128, 128), 128)]
        return pltpu.make_async_remote_copy(
            src_ref=block,
            dst_ref=block,
            send_sem=wo_s.at[sem],
            recv_sem=wo_r.at[sem],
            device_id=(row, target),
            device_id_type=MESH,
        )

    parts = (pl.ds(0, 672), pl.ds(672, 352))

    def wout_out(k):
        for d in (1, 3, 2):
            wout_copy(parts[k], col, lax.rem(chip + d, 4) * 2 + core, k).start()

    def wout_on(k):
        wait_for(wout_v.at[parts[k], pl.ds(0, 384)], wo_r.at[k])
        for d in (1, 2, 3):
            wout_copy(parts[k], lax.rem(chip + d, 4) * 2 + core, mate, 2).start()

    loads[3].wait()
    wout_out(0)
    wout_copy(pl.ds(0, 1024), col, mate, 2).start()

    project(1)
    row_exchange(send1.at[1], recv1.at[1], s1.at[1], r1.at[1])

    iota_row = lax.broadcasted_iota(jnp.int32, (512, 512), 0)
    iota_col = lax.broadcasted_iota(jnp.int32, (512, 512), 1)

    def chosen(hit):
        return jnp.where(hit, 1.0, 0.0).astype(BF16)

    perm_v[...] = chosen(
        iota_row == (iota_col % 32) * 16 + (iota_col // 64) * 2 + (iota_col % 64) // 32
    )
    pair = iota_row // 16
    chan = jnp.where(iota_row % 2 == 0, pair, jnp.where(pair == 0, 32, 64 - pair))
    loads[8].wait()
    wspec_p[...] = dot(
        chosen(iota_col == (iota_row % 16) // 2 * 64 + chan), wspec_v[...]
    ).astype(BF16)
    eye_v[...] = jnp.where(
        lax.broadcasted_iota(jnp.int32, (128, 128), 0)
        == lax.broadcasted_iota(jnp.int32, (128, 128), 1),
        1.0,
        0.0,
    ).astype(BF16)

    loads[7].wait()
    for b in range(2):
        wide = x_v[b, col // 2, pl.ds(pl.multiple_of((col % 2) * 256, 256), 256), :].astype(F32)
        inv = lax.rsqrt(jnp.sum(wide * wide, axis=1, keepdims=True) * (1.0 / 1024) + EPS)
        normed = (wide * inv * gain_v[...]).astype(BF16)
        sig_v[b] = jax.nn.sigmoid(dot(normed, wgate_v[...]))

    loads[4].wait()
    loads[5].wait()
    loads[6].wait()
    plain = row != 0
    mix01 = jnp.where(plain, 1.0, 0.0).astype(F32)
    mix11 = jnp.where(plain, -1.0, 1.0).astype(F32)
    odd = jnp.where(plain, 1, 0)

    def transform(b):
        section = dot(first_v[...], recv1[b])
        c = twist_v[0]
        s = twist_v[1]

        def turned(re, im):
            return jnp.concatenate([re * c + im * s, im * c - re * s], axis=1).astype(BF16)

        even_part = dot_nt(second_v[0], turned(section[0:256], section[256:512]))
        odd_part = dot_nt(second_v[odd], turned(section[512:768], section[768:1024]))
        one = even_part + mix01 * odd_part
        two = mix01 * even_part + mix11 * odd_part
        both = (
            jnp.concatenate([one.reshape(8, 32, 256), two.reshape(8, 32, 256)], axis=1)
            .reshape(512, 256)
            .astype(BF16)
        )
        for h in range(2):
            send2[b, h] = both[:, h * 128 : (h + 1) * 128]
            col_exchange(send2.at[b, h], recv2.at[b, h], s2.at[b, h], r2.at[b, h])

    def rows64(i):
        return pl.ds(pl.multiple_of(i * 64, 64), 64)

    def col_exchange(src, dst, send_sem, recv_sem):
        def send(d, c):
            t = col_peer(d)
            pltpu.make_async_remote_copy(
                src_ref=src.at[rows64(t), :],
                dst_ref=dst.at[rows64(col), :],
                send_sem=send_sem,
                recv_sem=recv_sem,
                device_id=(row, t),
                device_id_type=MESH,
            ).start()
            return c

        lax.fori_loop(1, COLS, send, 0)
        dst[rows64(col), :] = src[rows64(col), :]

    def give_back(b, h):
        wait_for(recv2.at[b, h, pl.ds(0, 448), :], r2.at[b, h])
        send3[b, h] = dot(perm_v[...], recv2[b, h]).astype(BF16)
        row_exchange(send3.at[b, h], recv3.at[b, h], s3.at[b, h], r3.at[b, h])

    def finish(b, h):
        row_wait(recv3.at[b, h], r3.at[b, h])
        spectrum = dot_nt(eye_v[...], recv3[b, h]).astype(BF16)
        mixed_pre = dot(spectrum, wspec_p[...]).astype(BF16).astype(F32)
        mixed = (sig_v[b, h * 128 : (h + 1) * 128] * mixed_pre).astype(BF16)
        result = dot(mixed, wout_v[...]).astype(BF16)
        for t in range(COLS):
            send4[b, h, t] = result[:, t * 128 : (t + 1) * 128]
        place = pl.ds(pl.multiple_of(col * 256 + h * 128, 128), 128)

        def send(d, c):
            t = col_peer(d)
            pltpu.make_async_remote_copy(
                src_ref=send4.at[b, h, t],
                dst_ref=out.at[b, place, :],
                send_sem=s4.at[b, h],
                recv_sem=r4.at[b, h],
                device_id=(row, t),
                device_id_type=MESH,
            ).start()
            return c

        lax.fori_loop(1, COLS, send, 0)
        out[b, place, :] = send4[b, h, col]

    row_wait(recv1.at[0], r1.at[0])
    transform(0)
    wout_out(1)
    give_back(0, 0)
    row_wait(recv1.at[1], r1.at[1])
    transform(1)
    give_back(0, 1)
    wout_on(0)
    wout_on(1)
    give_back(1, 0)
    give_back(1, 1)
    wait_for(wout_v.at[:, pl.ds(0, 512)], wo_r.at[2])
    finish(0, 0)
    finish(0, 1)
    finish(1, 0)
    finish(1, 1)

    for b in range(2):
        row_wait(send1.at[b], s1.at[b])
        for h in range(2):
            wait_for(send2.at[b, h, pl.ds(0, 448), :], s2.at[b, h])
            row_wait(send3.at[b, h], s3.at[b, h])
            wait_for(send4.at[b, h, pl.ds(0, 7)], s4.at[b, h])
            wait_for(out.at[b, pl.ds(0, 896), :], r4.at[b, h])
    for k in range(2):
        wait_for(wout_v.at[parts[k], pl.ds(0, 384)], wo_s.at[k])
    wait_for(wout_v.at[:, pl.ds(0, 512)], wo_s.at[2])


def on_device(tokens, norm_gain, w_fourier_in, w_gate, w_spectrum, w_output):
    spread, first, twist, second = tables()
    vmem = pltpu.VMEM
    return pl.pallas_call(
        kernel,
        out_shape=vmem((2, 2048, 128), BF16),
        in_specs=[pl.BlockSpec(memory_space=pl.ANY)] * 10,
        out_specs=pl.BlockSpec(memory_space=pltpu.VMEM),
        scratch_shapes=[
            vmem((2, 4, 512, 1024), BF16),
            vmem((1, 1024), F32),
            vmem((64, 1024), BF16),
            vmem((1024, 1024), BF16),
            vmem((512, 1024), BF16),
            vmem((512, 1024), BF16),
            vmem((1024, 1024), BF16),
            vmem((512, 512), BF16),
            vmem((1024, 512), BF16),
            vmem((2, 256, 256), F32),
            vmem((2, 256, 512), BF16),
            vmem((64, 1024), BF16),
            vmem((2, 256, 512), BF16),
            vmem((2, 256, 1024), F32),
            vmem((512, 512), BF16),
            vmem((128, 128), BF16),
            vmem((2, 512, 256), BF16),
            vmem((2, 512, 256), BF16),
            *[vmem((2, 2, 512, 128), BF16)] * 4,
            vmem((2, 2, 8, 128, 128), BF16),
            pltpu.SemaphoreType.DMA((2, 4)),
            pltpu.SemaphoreType.DMA((9,)),
            pltpu.SemaphoreType.DMA((2,)),
            pltpu.SemaphoreType.DMA((2,)),
            *[pltpu.SemaphoreType.DMA((2, 2))] * 6,
            pltpu.SemaphoreType.DMA((3,)),
            pltpu.SemaphoreType.DMA((3,)),
        ],
        compiler_params=pltpu.CompilerParams(
            collective_id=0, has_side_effects=True, vmem_limit_bytes=60 << 20
        ),
    )(
        tokens, norm_gain.reshape(1, 1024), w_fourier_in.T, w_gate, w_spectrum, w_output,
        spread, first, twist, second,
    )


def solution(mesh):
    placed = (P(None, "row", None), P(), P(None, "col"), P(), P(), P(None, "col"))
    return jax.shard_map(
        on_device, mesh=mesh, in_specs=placed, out_specs=P(None, "row", "col"), check_vma=False
    )
```
